512 devices in a mesh: grp: 2 (over y), fs: 16 (over z), tp: 16 (over x, core).
Axes of the slice: x: 8, y: 2, z: 16, core: 2. Of those that a mesh axis runs over, the one named last changes fastest.
The devices are a block of a 8x16x16 slice.
Arguments:
- tokens: bfloat16 [4096, 2048], P(('grp', 'fs'), 'tp'), parts along dimension 0, may hold values from -40 to 40
- norm_gain: float32 [2048], P('tp'), may hold values from 0.1 to 1.9
- expert_ids: int32 [4096, 8], P(('grp', 'fs')), parts along dimension 0, may hold values from 0 to 63, all different within a row; in each aligned block of 128 rows (0 to 127, 128 to 255, ...) at most 24 rows name the same one
- route_scores: float32 [4096, 8], P(('grp', 'fs')), parts along dimension 0, may hold values from 0.1 to 1
- gate_weight: float32 [64, 512, 2048], P(None, 'fs', 'tp'), may hold values from -0.125 to 0.125
- up_weight: float32 [64, 512, 2048], P(None, 'fs', 'tp'), may hold values from -0.125 to 0.125
- down_weight: float32 [64, 512, 2048], P(None, 'fs', 'tp'), may hold values from -0.25 to 0.25
- shared_gate: float32 [512, 2048], P('fs', 'tp'), may hold values from -0.125 to 0.125
- shared_up: float32 [512, 2048], P('fs', 'tp'), may hold values from -0.125 to 0.125
- shared_down: float32 [512, 2048], P('fs', 'tp'), may hold values from -0.25 to 0.25
Outputs:
- gate_served: bfloat16 [128, 512, 2048], P(('grp', 'fs'), None, 'tp'), parts along dimension 0
- up_served: bfloat16 [128, 512, 2048], P(('grp', 'fs'), None, 'tp'), parts along dimension 0
- down_served: bfloat16 [128, 512, 2048], P(('grp', 'fs'), None, 'tp'), parts along dimension 0
- shared_gate_served: bfloat16 [1024, 2048], P('grp', 'tp'), parts along dimension 0
- shared_up_served: bfloat16 [1024, 2048], P('grp', 'tp'), parts along dimension 0
- shared_down_served: bfloat16 [1024, 2048], P('grp', 'tp'), parts along dimension 0
- layer_output: bfloat16 [4096, 2048], P(('grp', 'fs'), 'tp'), parts along dimension 0
The draws below stay inside these ranges and needn't reach their ends.
There are 2 independent parts, one for each index of `grp`. The reference program is written for one: setup_inputs(seed, part) draws one part's arguments, and reference() takes and returns one part's arrays. A program takes and returns all parts, laid end to end along the dimension named above; an argument that names none is the same for every part. Nothing has to cross between parts.
Inputs may be any that keep to these rules, and one draw needn't show every extreme that they name: `expert_ids`: each row names 8 different experts. Among the rows of one index of fs no expert is named more than 24 times; in every draw some expert reaches 24 on some index of fs.
All inputs are finite; a program needn't handle non-finite values.
Results may differ from the reference program's by a relative error of at most 0.03.
Values may be sent and summed in bfloat16 or wider, within the bound.
No kernel may reach another device: no remote copies, remote signals or barrier semaphores. Data moves between devices by JAX's collectives and lax.ppermute only.
A program may use at most 64 MiB of HBM per device.

```python
import math
import jax
import jax.numpy as jnp
import numpy as np
from jax import lax

D = 2048
FF = 512
EXPERTS = 64
TOP_K = 8
TOK_DEV = 128
CAPACITY = 24
TOKENS = 2048
N_FS = 16
N_TP = 16


def draw_tokens(key, part):
    draw_key = jax.random.fold_in(key, 0)
    column = 3.0 ** (jnp.arange(D, dtype=jnp.float32) / (D - 1))
    values = jnp.clip(jax.random.normal(draw_key, (TOKENS, D), jnp.float32), -8.0, 8.0)
    return (values * column[None, :]).astype(jnp.bfloat16)


def levels(rng, extent, cuts, smallest, top_value):
    def one(dim, shards_of):
        heights = jax.random.uniform(jax.random.fold_in(jax.random.fold_in(rng, 6), dim), (shards_of,), jnp.float32, smallest / len(cuts), top_value / len(cuts))
        return jnp.repeat(jnp.exp(heights), extent[dim] // shards_of).reshape((-1,) + (1,) * (len(extent) - dim - 1))

    loudness = one(*cuts[0])
    for cut in cuts[1:]:
        loudness = loudness * one(*cut)
    return loudness


def assign_block(stream_key, own, number, rows, number_of, top, most, lean):
    sequence = jax.random.permutation(stream_key, number_of)
    heavy_load, common = load_shares(number_of, rows * top, most, lean, True), load_shares(number_of, rows * top, most, lean, False)
    places = jnp.arange(number_of)

    def named(lengths, rotation):
        used = int((lengths > 0).sum())
        fixed = max(1, used // 4)
        passed = fixed + (places - fixed + rotation * (used - fixed)) % max(1, number_of - fixed)
        return jnp.zeros((number_of,), jnp.int32).at[sequence[jnp.where(places < fixed, places, passed)]].set(jnp.asarray(lengths, jnp.int32))

    lengths = jnp.where(number % 4 == 0, named(heavy_load, number // 4), named(common, number - number // 4 - 1))
    mixed = jax.random.permutation(jax.random.fold_in(own, 3), number_of)
    source_of, receiver = mixed[0:number_of // 2 * 2:2], mixed[1:number_of // 2 * 2:2]
    margin = jnp.minimum(lengths[source_of] - 1, most - lengths[receiver]) // 2
    margin = jnp.where((source_of == sequence[0]) | (receiver == sequence[0]) | (lengths[receiver] == 0), 0, jnp.maximum(margin, 0))
    passed = jax.random.randint(jax.random.fold_in(own, 4), (number_of // 2,), 0, 1 << 20) % (margin + 1)
    lengths = lengths.at[source_of].add(-passed).at[receiver].add(passed)
    members = jnp.searchsorted(jnp.cumsum(lengths), jnp.arange(rows * top), side="right").astype(jnp.int32)
    table = members.reshape(top, rows).T
    table = table[jax.random.permutation(jax.random.fold_in(own, 1), rows)]
    rotation = jax.random.randint(jax.random.fold_in(own, 2), (rows, 1), 0, top)
    return jnp.take_along_axis(table, (jnp.arange(top)[None, :] + rotation) % top, axis=1)


def load_shares(amount, total, most, lean, full):
    loads = [(1 << 20) // math.isqrt(standing ** lean) + 1 for standing in range(1, amount + 1)]
    largest = most if full else min(most, max(-(-total // amount), total * loads[0] // sum(loads)))
    least = 1 if total - largest >= amount - 1 else 0
    counts, spare = [largest] + [least] * (amount - 1), total - largest - least * (amount - 1)
    while spare > 0:
        movable = [i for i in range(1, amount) if counts[i] < largest] or [i for i in range(1, amount) if counts[i] < most]
        mass, remaining = sum([loads[i] for i in movable]), spare
        for i in movable:
            addition = min(most - counts[i], max(1, remaining * loads[i] // mass), spare)
            counts[i] = counts[i] + addition
            spare = spare - addition
    return np.array(counts)


def centred(key, shape, deviation, limit, cuts=(), kind=jnp.bfloat16):
    level = levels(key, shape, cuts, -0.22, 0.18) if cuts else 1.0
    array = jax.random.normal(key, shape, jnp.float32) * deviation * level
    return jnp.minimum(jnp.maximum(array, -limit), limit).astype(kind)


def setup_inputs(seed: int = 0, part: int = 0) -> dict:
    key_of = jax.random.split(jax.random.key(seed), 11)
    own_keys = jax.random.split(jax.random.fold_in(key_of[10], part), 11)
    tokens = draw_tokens(jax.random.fold_in(jax.random.fold_in(key_of[10], part), 71), part)
    norm_gain = jnp.clip(1.0 + 0.18 * jax.random.normal(key_of[1], (D,), jnp.float32), 0.1, 1.9)
    expert_ids_keys = jax.random.split(jax.random.fold_in(own_keys[2], 1), TOKENS // TOK_DEV)
    expert_ids_turns = jax.random.permutation(jax.random.fold_in(own_keys[2], 3), TOKENS // TOK_DEV)
    expert_ids = jax.vmap(lambda own, number: assign_block(jax.random.fold_in(own_keys[2], 2), own, number, TOK_DEV, EXPERTS, TOP_K, CAPACITY, 2))(expert_ids_keys, expert_ids_turns).reshape((TOKENS, TOP_K))
    route_scores = jnp.clip(jnp.exp(math.log(1.0) - 2.3025851 * jax.random.uniform(own_keys[3], (TOKENS, TOP_K), jnp.float32) ** levels(own_keys[3], (TOKENS, TOP_K), ((0, 16),), -0.2, 0.2)), 0.1, 1.0)
    gate_weight = centred(key_of[4], (EXPERTS, FF, D), D ** -0.5, 0.125, ((1, 16), (2, 16)), jnp.float32)
    up_weight = centred(key_of[5], (EXPERTS, FF, D), D ** -0.5, 0.125, ((1, 16), (2, 16)), jnp.float32)
    down_weight = centred(key_of[6], (EXPERTS, FF, D), FF ** -0.5, 0.25, ((1, 16), (2, 16)), jnp.float32)
    shared_gate = centred(key_of[7], (FF, D), D ** -0.5, 0.125, ((0, 16), (1, 16)), jnp.float32)
    shared_up = centred(key_of[8], (FF, D), D ** -0.5, 0.125, ((0, 16), (1, 16)), jnp.float32)
    shared_down = centred(key_of[9], (FF, D), FF ** -0.5, 0.25, ((0, 16), (1, 16)), jnp.float32)
    return dict(tokens=tokens, norm_gain=norm_gain, expert_ids=expert_ids, route_scores=route_scores, gate_weight=gate_weight, up_weight=up_weight, down_weight=down_weight, shared_gate=shared_gate, shared_up=shared_up, shared_down=shared_down)


norm_eps = 1e-05
routed_scale = 2.5

def normalize(tokens):
    tok_float = tokens.astype(jnp.float32)
    full_width = tok_float.shape[1]
    row_mean = lax.optimization_barrier(jnp.sum(tok_float, axis=1)) / full_width
    row_var = lax.optimization_barrier(jnp.sum(tok_float * tok_float, axis=1)) / full_width - row_mean * row_mean
    return ((tok_float - row_mean[:, None]) * lax.rsqrt(row_var + norm_eps)[:, None]).astype(jnp.bfloat16)

def blocked_hidden(rows_in, paired):
    count_rows = rows_in.shape[0]
    split_rows = rows_in.astype(jnp.float32).reshape(count_rows, N_TP, -1)
    split_pair = paired.astype(jnp.float32).reshape(paired.shape[0], N_TP, -1)
    partial_value = jnp.einsum('ntd,ftd->tnf', split_rows, split_pair).astype(jnp.bfloat16)
    summed = lax.optimization_barrier(jnp.sum(partial_value.astype(jnp.float32), axis=0))
    return (jax.nn.silu(summed[:, :FF]) * summed[:, FF:]).astype(jnp.bfloat16)

def reference(tokens, norm_gain, expert_ids, route_scores, gate_weight, up_weight, down_weight, shared_gate, shared_up, shared_down):
    normed = normalize(tokens)
    gate_new = (gate_weight * norm_gain[None, None, :]).astype(jnp.bfloat16)
    up_new = (up_weight * norm_gain[None, None, :]).astype(jnp.bfloat16)
    down_new = down_weight.astype(jnp.bfloat16)
    gate_shared = (shared_gate * norm_gain[None, :]).astype(jnp.bfloat16)
    up_shared = (shared_up * norm_gain[None, :]).astype(jnp.bfloat16)
    down_shared = shared_down.astype(jnp.bfloat16)
    route_weight = route_scores / lax.optimization_barrier(jnp.sum(route_scores, axis=1, keepdims=True)) * routed_scale
    flat_ids = expert_ids.reshape(-1)
    assignments = flat_ids.shape[0]
    flat_tokens = jnp.concatenate([jnp.arange(assignments, dtype=jnp.int32) // TOP_K, jnp.full((1,), TOKENS, jnp.int32)])
    flat_weight = jnp.concatenate([route_weight.reshape(-1), jnp.zeros((1,), jnp.float32)])
    padded = jnp.concatenate([normed, jnp.zeros((1, D), jnp.bfloat16)], axis=0)

    def one_expert(running, expert):
        chosen = jnp.nonzero(flat_ids == expert, size=N_FS * CAPACITY, fill_value=assignments)[0].astype(jnp.int32)
        token_rows = flat_tokens[chosen]
        paired = jnp.concatenate([gate_new[expert], up_new[expert]], axis=0)
        hidden = blocked_hidden(padded[token_rows], paired)
        result = jnp.dot(hidden, down_new[expert], preferred_element_type=jnp.float32).astype(jnp.bfloat16)
        return (running.at[token_rows].add(result.astype(jnp.float32) * flat_weight[chosen][:, None]), None)
    routed, _ = lax.scan(one_expert, jnp.zeros((TOKENS + 1, D), jnp.float32), jnp.arange(EXPERTS, dtype=jnp.int32))
    shared_hidden = blocked_hidden(normed, jnp.concatenate([gate_shared, up_shared], axis=0))
    shared_out = jnp.dot(shared_hidden, down_shared, preferred_element_type=jnp.float32)
    layer_out = (shared_out + routed[:TOKENS]).astype(jnp.bfloat16)
    return (gate_new, up_new, down_new, gate_shared, up_shared, down_shared, layer_out)
```

```python
import jax
import jax.numpy as jnp
from jax import lax
from jax.sharding import Mesh
from jax.sharding import PartitionSpec as P

CAPACITY = 24
TP = ("tp_0", "tp_1")


norm_eps = 1e-05
routed_scale = 2.5


def exchange(array, axis):
    return lax.all_to_all(array, axis, 0, 0, tiled=True)


def copy_for_each(array, axis):
    size = lax.axis_size(axis)
    return exchange(jnp.broadcast_to(array[None], (size, *array.shape)), axis)


def swap_cores(array):
    return lax.ppermute(array, "tp_1", [(0, 1), (1, 0)])


def of_core(array, core, dim):
    half = array.shape[dim] // 2
    return lax.dynamic_slice_in_dim(array, core * half, half, axis=dim)


def with_shared(routed, shared, shards):
    experts, rows, width = routed.shape
    return jnp.concatenate(
        [
            routed.reshape(shards, experts // shards, rows, width),
            jnp.broadcast_to(shared[None, None], (shards, 1, rows, width)),
        ],
        axis=1,
    )


def by_expert(arrived):
    shards, experts, rows, width = arrived.shape
    return arrived.transpose(1, 0, 2, 3).reshape(experts, shards * rows, width)


def on_device(
    tokens,
    norm_gain,
    expert_ids,
    route_scores,
    gate_weight,
    up_weight,
    down_weight,
    shared_gate,
    shared_up,
    shared_down,
):
    shards = lax.axis_size("fs")
    chips = lax.axis_size("tp_0")
    core = lax.axis_index("tp_1")
    experts_all = gate_weight.shape[0]
    experts_here = experts_all // shards
    experts_core = experts_here // 2
    tok_rows, slice_width = tokens.shape
    tok_half = tok_rows // 2

    gain = norm_gain[None, None, :]
    gate_new = (gate_weight * gain).astype(jnp.bfloat16)
    up_new = (up_weight * gain).astype(jnp.bfloat16)
    down_new = down_weight.astype(jnp.bfloat16)
    gate_shared = (shared_gate * norm_gain[None, :]).astype(jnp.bfloat16)
    up_shared = (shared_up * norm_gain[None, :]).astype(jnp.bfloat16)
    down_shared = shared_down.astype(jnp.bfloat16)
    both_sent = jnp.stack(
        [with_shared(gate_new, gate_shared, shards), with_shared(up_new, up_shared, shards)], axis=1
    )
    both_here = exchange(both_sent, "fs")
    gate_all = by_expert(both_here[:, 0])
    up_all = by_expert(both_here[:, 1])

    tok_both = jnp.concatenate([tokens, swap_cores(tokens)], axis=1).astype(jnp.float32)
    sums = jnp.stack([jnp.sum(tok_both, axis=1), jnp.sum(tok_both * tok_both, axis=1)])
    row_sum, row_squares = copy_for_each(sums, "tp_0").sum(axis=0)
    full_width = slice_width * lax.axis_size(TP)
    row_mean = row_sum / full_width
    row_var = row_squares / full_width - row_mean * row_mean
    normed = ((tok_both - row_mean[:, None]) * lax.rsqrt(row_var + norm_eps)[:, None]).astype(
        jnp.bfloat16
    )

    route_weight = route_scores / jnp.sum(route_scores, axis=1, keepdims=True) * routed_scale
    named = expert_ids.T[:, None, :] == jnp.arange(experts_all, dtype=jnp.int32)[None, :, None]
    chosen = jnp.any(named, axis=0)
    weight_of = jnp.sum(jnp.where(named, route_weight.T[:, None, :], 0.0), axis=0)
    before = (
        jnp.arange(tok_rows, dtype=jnp.int32)[:, None] < jnp.arange(tok_rows, dtype=jnp.int32)[None, :]
    )
    rank = jnp.dot(
        chosen.astype(jnp.bfloat16), before.astype(jnp.bfloat16), preferred_element_type=jnp.float32
    )
    slot = jnp.where(chosen, rank.astype(jnp.int32), -1)
    slot = of_core(slot.reshape(shards, experts_here, tok_rows), core, 1)
    weight_of = of_core(weight_of.reshape(shards, experts_here, tok_rows), core, 1)
    in_slot = slot[:, :, None, :] == jnp.arange(CAPACITY, dtype=jnp.int32)[None, None, :, None]
    core_rows = shards * experts_core * CAPACITY
    select = in_slot.astype(jnp.bfloat16).reshape(core_rows, tok_rows)
    combine = jnp.where(in_slot, weight_of[:, :, None, :], 0.0).reshape(core_rows, tok_rows)

    outgoing = jnp.dot(select, normed, preferred_element_type=jnp.float32).astype(jnp.bfloat16)
    arrived = exchange(outgoing.reshape(shards, experts_core, CAPACITY, 2 * slice_width), "fs")
    rows_in = by_expert(arrived)

    hidden_width = gate_all.shape[1]
    paired = jnp.concatenate([gate_all, up_all], axis=1)

    def over_both(local, axis):
        mine = jnp.concatenate([of_core(local[:experts_here], core, 0), local[experts_here:]])
        theirs = jnp.concatenate([of_core(local[:experts_here], 1 - core, 0), local[experts_here:]])
        return jnp.concatenate([mine, swap_cores(theirs)], axis=axis)

    paired = over_both(paired, 2)
    routed_terms = jnp.einsum(
        "erd,efd->erf", rows_in, paired[:experts_core], preferred_element_type=jnp.float32
    ).astype(jnp.bfloat16)
    shared_terms = lax.dot_general(
        of_core(normed, core, 0),
        paired[experts_core],
        (((1,), (1,)), ((), ())),
        preferred_element_type=jnp.float32,
    ).astype(jnp.bfloat16)
    all_terms = jnp.concatenate(
        [routed_terms.reshape(core_rows, 2 * hidden_width), shared_terms], axis=0
    )
    part_rows = all_terms.shape[0] // chips
    parts = exchange(all_terms.reshape(chips, part_rows, 2 * hidden_width), "tp_0")
    row_share = jnp.sum(parts.astype(jnp.float32), axis=0)
    hidden_part = (jax.nn.silu(row_share[:, :hidden_width]) * row_share[:, hidden_width:]).astype(
        jnp.bfloat16
    )
    hidden = copy_for_each(hidden_part, "tp_0").reshape(chips * part_rows, hidden_width)

    down_all = by_expert(exchange(with_shared(down_new, down_shared, shards), "fs"))
    down_both = over_both(down_all, 2)
    outputs = jnp.einsum(
        "erf,efd->erd",
        hidden[:core_rows].reshape(experts_core, shards * CAPACITY, hidden_width),
        down_both[:experts_core],
        preferred_element_type=jnp.float32,
    ).astype(jnp.bfloat16)
    returned = exchange(
        outputs.reshape(experts_core, shards, CAPACITY, 2 * slice_width).transpose(1, 0, 2, 3), "fs"
    ).reshape(core_rows, 2 * slice_width)
    routed = lax.dot_general(
        combine,
        returned.astype(jnp.float32),
        (((0,), (0,)), ((), ())),
        precision=lax.Precision.HIGHEST,
        preferred_element_type=jnp.float32,
    )
    shared_out = jnp.dot(hidden[core_rows:], down_both[experts_core], preferred_element_type=jnp.float32)
    half_rows = jnp.arange(tok_rows, dtype=jnp.int32)[:, None] // tok_half == core
    total = routed + jnp.where(half_rows, jnp.concatenate([shared_out, shared_out], axis=0), 0.0)
    layer_out = (total[:, :slice_width] + swap_cores(total[:, slice_width:])).astype(jnp.bfloat16)
    return (
        gate_all[:experts_here],
        up_all[:experts_here],
        down_all[:experts_here],
        gate_all[experts_here],
        up_all[experts_here],
        down_all[experts_here],
        layer_out,
    )


def solution(mesh):
    split = Mesh(
        mesh.devices.reshape(mesh.shape["grp"], mesh.shape["fs"], mesh.shape["tp"] // 2, 2),
        ("grp", "fs", "tp_0", "tp_1"),
    )
    return jax.shard_map(
        on_device,
        mesh=split,
        in_specs=(
            P(("grp", "fs"), TP),
            P(TP),
            P(("grp", "fs"), None),
            P(("grp", "fs"), None),
            P(None, "fs", TP),
            P(None, "fs", TP),
            P(None, "fs", TP),
            P("fs", TP),
            P("fs", TP),
            P("fs", TP),
        ),
        out_specs=(
            P(("grp", "fs"), None, TP),
            P(("grp", "fs"), None, TP),
            P(("grp", "fs"), None, TP),
            P("grp", TP),
            P("grp", TP),
            P("grp", TP),
            P(("grp", "fs"), TP),
        ),
        check_vma=False,
    )
```

```python
import jax
import jax.numpy as jnp
from jax import lax
from jax.sharding import Mesh
from jax.sharding import PartitionSpec as P

CAPACITY = 24
TP = ("tp_0", "tp_1")


norm_eps = 1e-05
routed_scale = 2.5


def exchange(array, axis):
    return lax.all_to_all(array, axis, 0, 0, tiled=True)


def rotated(array, axis, by):
    size = lax.axis_size(axis)
    return lax.ppermute(array, axis, [(i, (i + by) % size) for i in range(size)])


def distances(axis):
    size = lax.axis_size(axis)
    return sorted(range(1, size), key=lambda by: -min(by, size - by))


def summed_parts(blocks, axis):
    at = lax.axis_index(axis)
    size = lax.axis_size(axis)
    pick = lambda i: lax.dynamic_index_in_dim(blocks, i % size, 0, keepdims=False)
    parts = [rotated(pick(at + by), axis, by) for by in distances(axis)]
    total = pick(at).astype(jnp.float32)
    for part in parts:
        total = total + part.astype(jnp.float32)
    return total


def of_all(array, axis):
    return {0: array, **{by: rotated(array, axis, by) for by in distances(axis)}}


def in_order(arrived, axis):
    at = lax.axis_index(axis)
    size = lax.axis_size(axis)
    out = jnp.zeros((size, *arrived[0].shape), arrived[0].dtype)
    for by, array in arrived.items():
        out = lax.dynamic_update_index_in_dim(out, array, (at - by) % size, 0)
    return out


def swap_cores(array):
    return lax.ppermute(array, "tp_1", [(0, 1), (1, 0)])


def of_core(array, core, dim):
    half = array.shape[dim] // 2
    return lax.dynamic_slice_in_dim(array, core * half, half, axis=dim)


def tie(array, after):
    return lax.optimization_barrier((array, after))[0]


def for_shards(weight, shards):
    experts, rows, width = weight.shape
    return weight.reshape(shards, 2, experts // shards // 2, rows, width)


def to_shards(routed, shared):
    if shared is None:
        return exchange(routed, "fs")
    rows = jnp.broadcast_to(shared[None, None], (routed.shape[0], 1, *shared.shape))
    return exchange(jnp.concatenate([routed, rows], axis=1), "fs")


def by_expert(arrived):
    shards, experts, rows, width = arrived.shape
    return arrived.transpose(1, 0, 2, 3).reshape(experts, shards * rows, width)


def on_device(
    tokens,
    norm_gain,
    expert_ids,
    route_scores,
    gate_weight,
    up_weight,
    down_weight,
    shared_gate,
    shared_up,
    shared_down,
):
    shards = lax.axis_size("fs")
    chips = lax.axis_size("tp_0")
    core = lax.axis_index("tp_1")
    experts_all = gate_weight.shape[0]
    experts_core = experts_all // shards // 2
    tok_rows, slice_width = tokens.shape
    tok_half = tok_rows // 2
    hidden_width = gate_weight.shape[1] * shards
    chunk_rows = shards * CAPACITY
    bf16 = jnp.bfloat16
    float32 = jnp.float32

    gain = norm_gain[None, None, :]
    gate_new = for_shards((gate_weight * gain).astype(bf16), shards)
    up_new = for_shards((up_weight * gain).astype(bf16), shards)
    down_new = down_weight.astype(bf16)
    both_shared = jnp.concatenate([shared_gate * gain[0], shared_up * gain[0]]).astype(bf16)
    down_shared = shared_down.astype(bf16)

    def both_new(i):
        return jnp.concatenate([gate_new[:, :, i], up_new[:, :, i]], axis=2)

    def halves(arrived):
        count, experts, rows, width = arrived.shape
        arranged = arrived.reshape(count, experts, 2, rows // 2, width).transpose(1, 2, 0, 3, 4)
        return arranged.reshape(experts, 2 * hidden_width, width)

    tok_both = jnp.concatenate([tokens, swap_cores(tokens)], axis=1).astype(float32)
    sums = jnp.stack([jnp.sum(tok_both, axis=1), jnp.sum(tok_both * tok_both, axis=1)])
    first_sent = both_new(0)
    first_here = to_shards(first_sent, both_shared)
    row_sum, row_squares = sum(of_all(sums, "tp_0").values())
    full_width = slice_width * lax.axis_size(TP)
    row_mean = row_sum / full_width
    row_var = row_squares / full_width - row_mean * row_mean
    normed = ((tok_both - row_mean[:, None]) * lax.rsqrt(row_var + norm_eps)[:, None]).astype(bf16)

    route_weight = route_scores / jnp.sum(route_scores, axis=1, keepdims=True) * routed_scale
    named = expert_ids.T[:, None, :] == jnp.arange(experts_all, dtype=jnp.int32)[None, :, None]
    chosen = jnp.any(named, axis=0)
    weight_of = jnp.sum(jnp.where(named, route_weight.T[:, None, :], 0.0), axis=0)
    places = jnp.arange(tok_rows, dtype=jnp.int32)
    before = places[:, None] < places[None, :]
    rank = jnp.dot(chosen.astype(bf16), before.astype(bf16), preferred_element_type=float32)
    slot = jnp.where(chosen, rank.astype(jnp.int32), -1)
    slot = of_core(slot.reshape(shards, 2 * experts_core, tok_rows), core, 1)
    weight_of = of_core(weight_of.reshape(shards, 2 * experts_core, tok_rows), core, 1)
    in_slot = slot[:, :, None, :] == jnp.arange(CAPACITY, dtype=jnp.int32)[None, None, :, None]
    select = in_slot.astype(bf16).reshape(experts_core * chunk_rows, tok_rows)

    outgoing = jnp.dot(select, normed, preferred_element_type=float32).astype(bf16)
    outgoing = outgoing.reshape(shards, experts_core, CAPACITY, 2 * slice_width)
    rows_in = by_expert(exchange(tie(outgoing, first_here), "fs"))

    def hidden_of(i, local, shared_local):
        own = lax.dynamic_index_in_dim(local, core, 0, keepdims=False)
        other = lax.dynamic_index_in_dim(local, 1 - core, 0, keepdims=False)
        if shared_local is None:
            pair = jnp.concatenate([own, swap_cores(other)], axis=1)
        else:
            swapped = swap_cores(jnp.concatenate([other, shared_local]))
            pair = jnp.concatenate([own, swapped[: 2 * hidden_width]], axis=1)
        over_width = (((1,), (1,)), ((), ()))
        terms = lax.dot_general(rows_in[i], pair, over_width, preferred_element_type=float32).astype(bf16)
        if shared_local is not None:
            pair = jnp.concatenate([shared_local, swapped[2 * hidden_width :]], axis=1)
            extra = lax.dot_general(
                of_core(normed, core, 0), pair, over_width, preferred_element_type=float32
            ).astype(bf16)
            terms = jnp.concatenate([terms, extra])
        part_rows = terms.shape[0] // chips
        share = summed_parts(terms.reshape(chips, part_rows, 2 * hidden_width), "tp_0")
        part = (jax.nn.silu(share[:, :hidden_width]) * share[:, hidden_width:]).astype(bf16)
        return in_order(of_all(part, "tp_0"), "tp_0").reshape(chips * part_rows, hidden_width)

    first_local = halves(first_here)
    both_whole = first_local[2]
    second_here = to_shards(tie(both_new(1), rows_in), None)
    hidden_first = hidden_of(0, first_local[:2], both_whole)
    second_here = tie(second_here, hidden_first)
    second_local = halves(second_here)
    down_sent = tie(down_new, second_here)
    down_sent = down_sent.reshape(shards, 2 * experts_core, *down_new.shape[1:])
    down_all = by_expert(to_shards(down_sent, down_shared))
    hidden_second = hidden_of(1, second_local, None)
    down_all = tie(down_all, hidden_second)
    down_whole = down_all[2 * experts_core]
    down_here = down_all[: 2 * experts_core]

    own = of_core(down_here, core, 0)
    swapped = swap_cores(jnp.concatenate([of_core(down_here, 1 - core, 0), down_whole[None]]))
    down_pair = jnp.concatenate([jnp.concatenate([own, down_whole[None]]), swapped], axis=2)

    def results(i, hidden, after):
        out = jnp.dot(hidden[:chunk_rows], down_pair[i], preferred_element_type=float32).astype(bf16)
        if after is not None:
            out = tie(out, after)
        back = exchange(out.reshape(shards, CAPACITY, 2 * slice_width), "fs")
        weights = jnp.where(in_slot[:, i], weight_of[:, i, None, :], 0.0)
        return back, lax.dot_general(
            weights.reshape(chunk_rows, tok_rows),
            back.reshape(chunk_rows, 2 * slice_width).astype(float32),
            (((0,), (0,)), ((), ())),
            precision=lax.Precision.HIGHEST,
            preferred_element_type=float32,
        )

    back, total = results(0, hidden_first, None)
    shared_out = jnp.dot(
        hidden_first[chunk_rows:], down_pair[experts_core], preferred_element_type=float32
    )
    half_rows = places[:, None] // tok_half == core
    total = total + jnp.where(half_rows, jnp.concatenate([shared_out, shared_out]), 0.0)
    total = total + results(1, hidden_second, back)[1]
    layer_out = (total[:, :slice_width] + swap_cores(total[:, slice_width:])).astype(bf16)

    served = jnp.stack([first_local[:2], second_local], axis=1)
    served = served.reshape(2 * experts_core, 2 * hidden_width, slice_width)
    return (
        served[:, :hidden_width],
        served[:, hidden_width:],
        down_here,
        both_whole[:hidden_width],
        both_whole[hidden_width:],
        down_whole,
        layer_out,
    )


def solution(mesh):
    split = Mesh(
        mesh.devices.reshape(mesh.shape["grp"], mesh.shape["fs"], mesh.shape["tp"] // 2, 2),
        ("grp", "fs", "tp_0", "tp_1"),
    )
    return jax.shard_map(
        on_device,
        mesh=split,
        in_specs=(
            P(("grp", "fs"), TP),
            P(TP),
            P(("grp", "fs"), None),
            P(("grp", "fs"), None),
            P(None, "fs", TP),
            P(None, "fs", TP),
            P(None, "fs", TP),
            P("fs", TP),
            P("fs", TP),
            P("fs", TP),
        ),
        out_specs=(
            P(("grp", "fs"), None, TP),
            P(("grp", "fs"), None, TP),
            P(("grp", "fs"), None, TP),
            P("grp", TP),
            P("grp", TP),
            P("grp", TP),
            P(("grp", "fs"), TP),
        ),
        check_vma=False,
    )
```

```python
import jax
import jax.numpy as jnp
from jax import lax
from jax.sharding import Mesh
from jax.sharding import PartitionSpec as P

CAPACITY = 24
TP = ("tp_0", "tp_1")


norm_eps = 1e-05
routed_scale = 2.5


def exchange(array, axis):
    return lax.all_to_all(array, axis, 0, 0, tiled=True)


def rotated(array, axis, by):
    size = lax.axis_size(axis)
    return lax.ppermute(array, axis, [(i, (i + by) % size) for i in range(size)])


def distances(axis):
    size = lax.axis_size(axis)
    return sorted(range(1, size), key=lambda by: -min(by, size - by))


def summed_parts(blocks, axis):
    at = lax.axis_index(axis)
    size = lax.axis_size(axis)
    pick = lambda i: lax.dynamic_index_in_dim(blocks, i % size, 0, keepdims=False)
    parts = [rotated(pick(at + by), axis, by) for by in distances(axis)]
    total = pick(at).astype(jnp.float32)
    for part in parts:
        total = total + part.astype(jnp.float32)
    return total


def swap_cores(array):
    return lax.ppermute(array, "tp_1", [(0, 1), (1, 0)])


def of_core(array, core, dim):
    half = array.shape[dim] // 2
    return lax.dynamic_slice_in_dim(array, core * half, half, axis=dim)


def tie(array, after):
    return lax.optimization_barrier((array, after))[0]


def to_shards(routed, shared):
    rows = jnp.broadcast_to(shared[None, None], (routed.shape[0], 1, *shared.shape))
    return exchange(jnp.concatenate([routed, rows], axis=1), "fs")


def by_expert(arrived):
    shards, experts, rows, width = arrived.shape
    return arrived.transpose(1, 0, 2, 3).reshape(experts, shards * rows, width)


def on_device(
    tokens,
    norm_gain,
    expert_ids,
    route_scores,
    gate_weight,
    up_weight,
    down_weight,
    shared_gate,
    shared_up,
    shared_down,
):
    shards = lax.axis_size("fs")
    chips = lax.axis_size("tp_0")
    core = lax.axis_index("tp_1")
    experts_all = gate_weight.shape[0]
    experts_here = experts_all // shards
    experts_core = experts_here // 2
    tok_rows, slice_width = tokens.shape
    tok_half = tok_rows // 2
    hidden_width = gate_weight.shape[1] * shards
    core_rows = experts_core * shards * CAPACITY
    bf16 = jnp.bfloat16
    float32 = jnp.float32

    gain = norm_gain[None, None, :]
    both_new = jnp.concatenate(
        [(gate_weight * gain).astype(bf16), (up_weight * gain).astype(bf16)], axis=1
    )
    both_shared = jnp.concatenate([shared_gate * gain[0], shared_up * gain[0]]).astype(bf16)
    both_sent = both_new.reshape(shards, experts_here, *both_new.shape[1:])
    both_arrived = to_shards(both_sent, both_shared)
    count, experts, rows, width = both_arrived.shape
    both_here = both_arrived.reshape(count, experts, 2, rows // 2, width).transpose(1, 2, 0, 3, 4)
    both_here = both_here.reshape(experts, 2 * hidden_width, width)

    tok_both = jnp.concatenate([tokens, swap_cores(tokens)], axis=1).astype(float32)
    sums = jnp.stack([jnp.sum(tok_both, axis=1), jnp.sum(tok_both * tok_both, axis=1)])
    row_sum, row_squares = jnp.sum(lax.all_gather(sums, "tp_0"), axis=0)
    full_width = slice_width * lax.axis_size(TP)
    row_mean = row_sum / full_width
    row_var = row_squares / full_width - row_mean * row_mean
    normed = ((tok_both - row_mean[:, None]) * lax.rsqrt(row_var + norm_eps)[:, None]).astype(bf16)

    route_weight = route_scores / jnp.sum(route_scores, axis=1, keepdims=True) * routed_scale
    named = expert_ids.T[:, None, :] == jnp.arange(experts_all, dtype=jnp.int32)[None, :, None]
    chosen = jnp.any(named, axis=0)
    weight_of = jnp.sum(jnp.where(named, route_weight.T[:, None, :], 0.0), axis=0)
    places = jnp.arange(tok_rows, dtype=jnp.int32)
    before = places[:, None] < places[None, :]
    rank = jnp.dot(chosen.astype(bf16), before.astype(bf16), preferred_element_type=float32)
    slot = jnp.where(chosen, rank.astype(jnp.int32), -1)
    slot = of_core(slot.reshape(shards, experts_here, tok_rows), core, 1)
    weight_of = of_core(weight_of.reshape(shards, experts_here, tok_rows), core, 1)
    in_slot = slot[:, :, None, :] == jnp.arange(CAPACITY, dtype=jnp.int32)[None, None, :, None]
    select = in_slot.astype(bf16).reshape(core_rows, tok_rows)
    combine = jnp.where(in_slot, weight_of[:, :, None, :], 0.0).reshape(core_rows, tok_rows)

    outgoing = jnp.dot(select, normed, preferred_element_type=float32).astype(bf16)
    outgoing = outgoing.reshape(shards, experts_core, CAPACITY, 2 * slice_width)
    arrived = exchange(tie(outgoing, both_arrived), "fs")
    rows_in = by_expert(arrived)

    down_sent = tie(down_weight.astype(bf16), arrived)
    down_sent = down_sent.reshape(shards, experts_here, *down_sent.shape[1:])
    down_arrived = to_shards(down_sent, shared_down.astype(bf16))

    def over_both(local, dim):
        mine = jnp.concatenate([of_core(local[:experts_here], core, 0), local[experts_here:]])
        theirs = jnp.concatenate([of_core(local[:experts_here], 1 - core, 0), local[experts_here:]])
        return jnp.concatenate([mine, swap_cores(theirs)], axis=dim)

    paired = over_both(both_here, 2)
    routed_terms = jnp.einsum(
        "erd,efd->erf", rows_in, paired[:experts_core], preferred_element_type=float32
    ).astype(bf16)
    shared_terms = lax.dot_general(
        of_core(normed, core, 0),
        paired[experts_core],
        (((1,), (1,)), ((), ())),
        preferred_element_type=float32,
    ).astype(bf16)
    all_terms = jnp.concatenate([routed_terms.reshape(core_rows, 2 * hidden_width), shared_terms])
    part_rows = all_terms.shape[0] // chips
    share = summed_parts(all_terms.reshape(chips, part_rows, 2 * hidden_width), "tp_0")
    part = (jax.nn.silu(share[:, :hidden_width]) * share[:, hidden_width:]).astype(bf16)
    hidden = lax.all_gather(part, "tp_0", axis=0, tiled=True)

    down_here = by_expert(tie(down_arrived, part))
    down_both = over_both(down_here, 2)
    outputs = jnp.einsum(
        "erf,efd->erd",
        hidden[:core_rows].reshape(experts_core, shards * CAPACITY, hidden_width),
        down_both[:experts_core],
        preferred_element_type=float32,
    ).astype(bf16)
    returned = exchange(
        outputs.reshape(experts_core, shards, CAPACITY, 2 * slice_width).transpose(1, 0, 2, 3), "fs"
    ).reshape(core_rows, 2 * slice_width)
    routed = lax.dot_general(
        combine,
        returned.astype(float32),
        (((0,), (0,)), ((), ())),
        precision=lax.Precision.HIGHEST,
        preferred_element_type=float32,
    )
    shared_out = jnp.dot(hidden[core_rows:], down_both[experts_core], preferred_element_type=float32)
    half_rows = places[:, None] // tok_half == core
    total = routed + jnp.where(half_rows, jnp.concatenate([shared_out, shared_out]), 0.0)
    layer_out = (total[:, :slice_width] + swap_cores(total[:, slice_width:])).astype(bf16)
    return (
        both_here[:experts_here, :hidden_width],
        both_here[:experts_here, hidden_width:],
        down_here[:experts_here],
        both_here[experts_here, :hidden_width],
        both_here[experts_here, hidden_width:],
        down_here[experts_here],
        layer_out,
    )


def solution(mesh):
    split = Mesh(
        mesh.devices.reshape(mesh.shape["grp"], mesh.shape["fs"], mesh.shape["tp"] // 2, 2),
        ("grp", "fs", "tp_0", "tp_1"),
    )
    return jax.shard_map(
        on_device,
        mesh=split,
        in_specs=(
            P(("grp", "fs"), TP),
            P(TP),
            P(("grp", "fs"), None),
            P(("grp", "fs"), None),
            P(None, "fs", TP),
            P(None, "fs", TP),
            P(None, "fs", TP),
            P("fs", TP),
            P("fs", TP),
            P("fs", TP),
        ),
        out_specs=(
            P(("grp", "fs"), None, TP),
            P(("grp", "fs"), None, TP),
            P(("grp", "fs"), None, TP),
            P("grp", TP),
            P("grp", TP),
            P("grp", TP),
            P(("grp", "fs"), TP),
        ),
        check_vma=False,
    )
```

```python
import jax
import jax.numpy as jnp
from jax import lax
from jax.sharding import Mesh
from jax.sharding import PartitionSpec as P

CAPACITY = 24
TP = ("tp_0", "tp_1")


norm_eps = 1e-05
routed_scale = 2.5


def exchange(array, axis):
    return lax.all_to_all(array, axis, 0, 0, tiled=True)


def rotated(array, axis, by):
    size = lax.axis_size(axis)
    return lax.ppermute(array, axis, [(i, (i + by) % size) for i in range(size)])


def distances(axis):
    size = lax.axis_size(axis)
    return sorted(range(1, size), key=lambda by: -min(by, size - by))


def summed_parts(blocks, axis):
    at = lax.axis_index(axis)
    size = lax.axis_size(axis)
    pick = lambda i: lax.dynamic_index_in_dim(blocks, i % size, 0, keepdims=False)
    parts = [rotated(pick(at + by), axis, by) for by in distances(axis)]
    total = pick(at).astype(jnp.float32)
    for part in parts:
        total = total + part.astype(jnp.float32)
    return total


def swap_cores(array):
    return lax.ppermute(array, "tp_1", [(0, 1), (1, 0)])


def of_core(array, core, dim):
    half = array.shape[dim] // 2
    return lax.dynamic_slice_in_dim(array, core * half, half, axis=dim)


def tie(array, after):
    return lax.optimization_barrier((array, after))[0]


def to_shards(routed, shared):
    rows = jnp.broadcast_to(shared[None, None], (routed.shape[0], 1, *shared.shape))
    return exchange(jnp.concatenate([routed, rows], axis=1), "fs")


def on_device(
    tokens,
    norm_gain,
    expert_ids,
    route_scores,
    gate_weight,
    up_weight,
    down_weight,
    shared_gate,
    shared_up,
    shared_down,
):
    shards = lax.axis_size("fs")
    chips = lax.axis_size("tp_0")
    core = lax.axis_index("tp_1")
    experts_all, unit_rows, slice_width = gate_weight.shape
    experts_here = experts_all // shards
    experts_core = experts_all // 2
    tok_rows, top_count = expert_ids.shape
    bf16 = jnp.bfloat16
    float32 = jnp.float32

    tok_float = tokens.astype(float32)
    sums = jnp.stack([jnp.sum(tok_float, axis=1), jnp.sum(tok_float * tok_float, axis=1)])
    row_sum, row_squares = jnp.sum(lax.all_gather(sums + swap_cores(sums), "tp_0"), axis=0)
    full_width = slice_width * lax.axis_size(TP)
    row_mean = row_sum / full_width
    row_var = row_squares / full_width - row_mean * row_mean
    normed = ((tok_float - row_mean[:, None]) * lax.rsqrt(row_var + norm_eps)[:, None]).astype(bf16)

    route_weight = route_scores / jnp.sum(route_scores, axis=1, keepdims=True) * routed_scale
    sent = jnp.concatenate([normed, expert_ids.T.astype(bf16), route_weight.T.astype(bf16)])
    blocks = lax.all_gather(sent, "fs")
    own_tokens = blocks[:, :tok_rows]
    all_tokens = jnp.concatenate([own_tokens, swap_cores(own_tokens)], axis=2)
    ids = blocks[:, tok_rows : tok_rows + top_count].astype(jnp.int32)
    weights = blocks[:, tok_rows + top_count :].astype(float32)

    gain = norm_gain[None, None, :]
    both_new = jnp.concatenate(
        [(gate_weight * gain).astype(bf16), (up_weight * gain).astype(bf16)], axis=1
    )
    both_shared = jnp.concatenate([shared_gate * gain[0], shared_up * gain[0]]).astype(bf16)
    down_new = down_weight.astype(bf16)
    down_shared = shared_down.astype(bf16)
    three_new = jnp.concatenate([both_new, down_new], axis=1)
    three_sent = tie(three_new, blocks).reshape(shards, experts_here, 3 * unit_rows, slice_width)
    served = to_shards(three_sent, jnp.concatenate([both_shared, down_shared]))

    def over_both(local, shared_local):
        rows = local.shape[1]
        mine = of_core(local, core, 0)
        theirs = jnp.concatenate([of_core(local, 1 - core, 0), shared_local[None]])
        theirs = swap_cores(theirs.reshape(-1, slice_width)).reshape(-1, rows, slice_width)
        routed = jnp.concatenate([mine, theirs[:-1]], axis=2)
        return routed, jnp.concatenate([shared_local, theirs[-1]], axis=1)

    both_pair, both_shared_pair = over_both(both_new, both_shared)
    down_pair, down_shared_pair = over_both(down_new, down_shared)

    core_experts = core * experts_core + jnp.arange(experts_core, dtype=jnp.int32)
    named = ids[:, :, None, :] == core_experts[None, None, :, None]
    chosen = jnp.any(named, axis=1)
    weight_of = jnp.sum(jnp.where(named, weights[:, :, None, :], 0.0), axis=1)
    places = jnp.arange(tok_rows, dtype=jnp.int32)
    before = places[:, None] < places[None, :]
    rank = jnp.einsum(
        "bet,tu->beu", chosen.astype(bf16), before.astype(bf16), preferred_element_type=float32
    )
    slot = jnp.where(chosen, rank.astype(jnp.int32), -1)
    in_slot = slot[:, :, None, :] == jnp.arange(CAPACITY, dtype=jnp.int32)[None, None, :, None]
    slots = experts_core * CAPACITY
    select = in_slot.astype(bf16).reshape(shards, slots, tok_rows)
    combine = jnp.where(in_slot, weight_of[:, :, None, :], 0.0).astype(bf16)
    combine = combine.reshape(shards, slots, tok_rows)

    rows_in = jnp.einsum(
        "brt,btd->brd", select, all_tokens, preferred_element_type=float32
    ).astype(bf16)
    rows_in = rows_in.reshape(shards, experts_core, CAPACITY, 2 * slice_width).transpose(1, 0, 2, 3)
    rows_in = rows_in.reshape(experts_core, shards * CAPACITY, 2 * slice_width)
    terms = jnp.einsum("efd,erd->efr", both_pair, rows_in, preferred_element_type=float32).astype(bf16)
    lanes = tok_rows
    groups = shards * CAPACITY // lanes
    terms = terms.reshape(chips, experts_core // chips, 2 * unit_rows, groups, lanes)
    terms = terms.transpose(0, 3, 1, 2, 4).reshape(chips, -1, lanes)
    shared_terms = jnp.einsum(
        "fd,btd->bft",
        both_shared_pair,
        of_core(all_tokens, core, 0),
        preferred_element_type=float32,
    ).astype(bf16)
    share = summed_parts(jnp.concatenate([terms, shared_terms], axis=1), "tp_0")
    share = share.reshape(-1, 2 * unit_rows, lanes)
    part = (jax.nn.silu(share[:, :unit_rows]) * share[:, unit_rows:]).astype(bf16)
    hidden = lax.all_gather(part.reshape(-1, lanes), "tp_0")
    hidden = hidden.reshape(chips, -1, unit_rows, lanes)

    routed_hidden = hidden[:, :-1].reshape(chips, groups, experts_core // chips, unit_rows, lanes)
    routed_hidden = routed_hidden.transpose(0, 2, 3, 1, 4)
    routed_hidden = routed_hidden.reshape(experts_core, unit_rows, groups * lanes)
    results = jnp.einsum(
        "efr,efd->erd", routed_hidden, down_pair, preferred_element_type=float32
    ).astype(bf16)
    results = results.reshape(experts_core, shards, CAPACITY, 2 * slice_width).transpose(1, 0, 2, 3)
    results = results.reshape(shards, slots, 2 * slice_width)
    total = jnp.einsum("brt,brd->btd", combine, results, preferred_element_type=float32)
    shared_out = jnp.einsum(
        "bft,fd->btd", hidden[:, -1], down_shared_pair, preferred_element_type=float32
    )
    halves = jnp.arange(shards, dtype=jnp.int32)[:, None, None] // (shards // 2) == core
    total = total + jnp.where(halves, jnp.concatenate([shared_out, shared_out]), 0.0)
    total = total[:, :, :slice_width] + swap_cores(
        total[:, :, slice_width:].astype(bf16).reshape(-1, slice_width)
    ).reshape(shards, tok_rows, slice_width).astype(float32)
    served = tie(served, hidden)
    partials = exchange(tie(total.astype(bf16), served), "fs")
    layer_out = jnp.sum(partials.astype(float32), axis=0).astype(bf16)

    served = served.reshape(shards, experts_here + 1, 3, unit_rows, slice_width)
    served = served.transpose(2, 1, 0, 3, 4).reshape(
        3, experts_here + 1, shards * unit_rows, slice_width
    )
    gate_here, up_here, down_here = served[0], served[1], served[2]
    return (
        gate_here[:experts_here],
        up_here[:experts_here],
        down_here[:experts_here],
        gate_here[experts_here],
        up_here[experts_here],
        down_here[experts_here],
        layer_out,
    )


def solution(mesh):
    split = Mesh(
        mesh.devices.reshape(mesh.shape["grp"], mesh.shape["fs"], mesh.shape["tp"] // 2, 2),
        ("grp", "fs", "tp_0", "tp_1"),
    )
    return jax.shard_map(
        on_device,
        mesh=split,
        in_specs=(
            P(("grp", "fs"), TP),
            P(TP),
            P(("grp", "fs"), None),
            P(("grp", "fs"), None),
            P(None, "fs", TP),
            P(None, "fs", TP),
            P(None, "fs", TP),
            P("fs", TP),
            P("fs", TP),
            P("fs", TP),
        ),
        out_specs=(
            P(("grp", "fs"), None, TP),
            P(("grp", "fs"), None, TP),
            P(("grp", "fs"), None, TP),
            P("grp", TP),
            P("grp", TP),
            P("grp", TP),
            P(("grp", "fs"), TP),
        ),
        check_vma=False,
    )
```

```python
import jax
import jax.numpy as jnp
from jax import lax
from jax.sharding import Mesh
from jax.sharding import PartitionSpec as P

CAPACITY = 24
TP = ("tp_0", "tp_1")


norm_eps = 1e-05
routed_scale = 2.5


def exchange(array, axis):
    return lax.all_to_all(array, axis, 0, 0, tiled=True)


def rotated(array, axis, by):
    size = lax.axis_size(axis)
    return lax.ppermute(array, axis, [(i, (i + by) % size) for i in range(size)])


def distances(axis):
    size = lax.axis_size(axis)
    return sorted(range(1, size), key=lambda by: -min(by, size - by))


def summed_parts(blocks, axis):
    at = lax.axis_index(axis)
    size = lax.axis_size(axis)
    pick = lambda i: lax.dynamic_index_in_dim(blocks, i % size, 0, keepdims=False)
    parts = [rotated(pick(at + by), axis, by) for by in distances(axis)]
    total = pick(at).astype(jnp.float32)
    for part in parts:
        total = total + part.astype(jnp.float32)
    return total


def swap_cores(array):
    return lax.ppermute(array, "tp_1", [(0, 1), (1, 0)])


def of_core(array, core, dim):
    half = array.shape[dim] // 2
    return lax.dynamic_slice_in_dim(array, core * half, half, axis=dim)


def copy_for_each(array, axis):
    size = lax.axis_size(axis)
    return exchange(jnp.broadcast_to(array[None], (size, *array.shape)), axis)


def tie(array, after):
    return lax.optimization_barrier((array, after))[0]


def with_shared(routed, shared):
    rows = jnp.broadcast_to(shared[None, None], (routed.shape[0], 1, *shared.shape))
    return jnp.concatenate([routed, rows], axis=1)


def on_device(
    tokens,
    norm_gain,
    expert_ids,
    route_scores,
    gate_weight,
    up_weight,
    down_weight,
    shared_gate,
    shared_up,
    shared_down,
):
    shards = lax.axis_size("fs")
    chips = lax.axis_size("tp_0")
    core = lax.axis_index("tp_1")
    experts_all, unit_rows, slice_width = gate_weight.shape
    experts_here = experts_all // shards
    experts_core = experts_all // 2
    tok_rows, top_count = expert_ids.shape
    bf16 = jnp.bfloat16
    float32 = jnp.float32

    tok_float = tokens.astype(float32)
    sums = jnp.stack([jnp.sum(tok_float, axis=1), jnp.sum(tok_float * tok_float, axis=1)])
    row_sum, row_squares = jnp.sum(copy_for_each(sums, TP), axis=0)
    full_width = slice_width * lax.axis_size(TP)
    row_mean = row_sum / full_width
    row_var = row_squares / full_width - row_mean * row_mean
    normed = ((tok_float - row_mean[:, None]) * lax.rsqrt(row_var + norm_eps)[:, None]).astype(bf16)

    route_weight = route_scores / jnp.sum(route_scores, axis=1, keepdims=True) * routed_scale
    sent = jnp.concatenate([normed, expert_ids.T.astype(bf16), route_weight.T.astype(bf16)])
    blocks = copy_for_each(sent, "fs")

    gain = norm_gain[None, None, :]
    both_new = jnp.concatenate(
        [(gate_weight * gain).astype(bf16), (up_weight * gain).astype(bf16)], axis=1
    )
    both_shared = jnp.concatenate([shared_gate * gain[0], shared_up * gain[0]]).astype(bf16)
    down_new = down_weight.astype(bf16)
    down_shared = shared_down.astype(bf16)
    three_new = jnp.concatenate([both_new, down_new], axis=1)
    three_sent = three_new.reshape(shards, experts_here, 3 * unit_rows, slice_width)
    three_sent = with_shared(three_sent, jnp.concatenate([both_shared, down_shared]))
    served = exchange(tie(three_sent, blocks), "fs")

    def over_both(local, shared_local):
        rows = local.shape[1]
        mine = of_core(local, core, 0)
        theirs = jnp.concatenate([of_core(local, 1 - core, 0), shared_local[None]])
        theirs = swap_cores(theirs.reshape(-1, slice_width)).reshape(-1, rows, slice_width)
        routed = jnp.concatenate([mine, theirs[:-1]], axis=2)
        return routed, jnp.concatenate([shared_local, theirs[-1]], axis=1)

    both_pair, both_shared_pair = over_both(both_new, both_shared)
    down_pair, down_shared_pair = over_both(down_new, down_shared)

    blocks = tie(blocks, (both_pair, both_shared_pair, down_pair, down_shared_pair))
    own_tokens = blocks[:, :tok_rows]
    all_tokens = jnp.concatenate([own_tokens, swap_cores(own_tokens)], axis=2)
    ids = blocks[:, tok_rows : tok_rows + top_count].astype(jnp.int32)
    weights = blocks[:, tok_rows + top_count :].astype(float32)

    core_experts = core * experts_core + jnp.arange(experts_core, dtype=jnp.int32)
    named = ids[:, :, None, :] == core_experts[None, None, :, None]
    chosen = jnp.any(named, axis=1)
    weight_of = jnp.sum(jnp.where(named, weights[:, :, None, :], 0.0), axis=1)
    places = jnp.arange(tok_rows, dtype=jnp.int32)
    before = places[:, None] < places[None, :]
    rank = jnp.einsum(
        "bet,tu->beu", chosen.astype(bf16), before.astype(bf16), preferred_element_type=float32
    )
    slot = jnp.where(chosen, rank.astype(jnp.int32), -1)
    in_slot = slot[:, :, None, :] == jnp.arange(CAPACITY, dtype=jnp.int32)[None, None, :, None]
    slots = experts_core * CAPACITY
    select = in_slot.astype(bf16).reshape(shards, slots, tok_rows)
    combine = jnp.where(in_slot, weight_of[:, :, None, :], 0.0).astype(bf16)
    combine = combine.reshape(shards, slots, tok_rows)

    rows_in = jnp.einsum(
        "brt,btd->brd", select, all_tokens, preferred_element_type=float32
    ).astype(bf16)
    rows_in = rows_in.reshape(shards, experts_core, CAPACITY, 2 * slice_width).transpose(1, 0, 2, 3)
    rows_in = rows_in.reshape(experts_core, shards * CAPACITY, 2 * slice_width)
    lanes = tok_rows
    groups = shards * CAPACITY // lanes

    def terms_of(group):
        rows = rows_in[:, group * lanes : (group + 1) * lanes]
        terms = jnp.einsum("efd,erd->efr", both_pair, rows, preferred_element_type=float32)
        return terms.astype(bf16).reshape(chips, -1, lanes)

    shared_terms = jnp.einsum(
        "fd,btd->bft",
        both_shared_pair,
        of_core(all_tokens, core, 0),
        preferred_element_type=float32,
    ).astype(bf16)
    share = summed_parts(jnp.concatenate([*map(terms_of, range(groups)), shared_terms], axis=1), "tp_0")
    share = share.reshape(-1, 2 * unit_rows, lanes)
    part = (jax.nn.silu(share[:, :unit_rows]) * share[:, unit_rows:]).astype(bf16)
    hidden = lax.all_gather(part.reshape(-1, lanes), "tp_0")
    hidden = hidden.reshape(chips, -1, unit_rows, lanes)

    routed_hidden = hidden[:, :-1].reshape(chips, groups, experts_core // chips, unit_rows, lanes)
    routed_hidden = routed_hidden.transpose(0, 2, 3, 1, 4)
    routed_hidden = routed_hidden.reshape(experts_core, unit_rows, groups * lanes)
    results = jnp.einsum(
        "efr,efd->erd", routed_hidden, down_pair, preferred_element_type=float32
    ).astype(bf16)
    results = results.reshape(experts_core, shards, CAPACITY, 2 * slice_width).transpose(1, 0, 2, 3)
    results = results.reshape(shards, slots, 2 * slice_width)
    total = jnp.einsum("brt,brd->btd", combine, results, preferred_element_type=float32)
    shared_out = jnp.einsum(
        "bft,fd->btd", hidden[:, -1], down_shared_pair, preferred_element_type=float32
    )
    halves = jnp.arange(shards, dtype=jnp.int32)[:, None, None] // (shards // 2) == core
    total = total + jnp.where(halves, jnp.concatenate([shared_out, shared_out]), 0.0)
    total = total[:, :, :slice_width] + swap_cores(
        total[:, :, slice_width:].astype(bf16).reshape(-1, slice_width)
    ).reshape(shards, tok_rows, slice_width).astype(float32)
    served = tie(served, hidden)
    partials = exchange(tie(total.astype(bf16), served), "fs")
    layer_out = jnp.sum(partials.astype(float32), axis=0).astype(bf16)

    served = served.reshape(shards, experts_here + 1, 3, unit_rows, slice_width)
    served = served.transpose(2, 1, 0, 3, 4).reshape(
        3, experts_here + 1, shards * unit_rows, slice_width
    )
    gate_here, up_here, down_here = served[0], served[1], served[2]
    return (
        gate_here[:experts_here],
        up_here[:experts_here],
        down_here[:experts_here],
        gate_here[experts_here],
        up_here[experts_here],
        down_here[experts_here],
        layer_out,
    )


def solution(mesh):
    split = Mesh(
        mesh.devices.reshape(mesh.shape["grp"], mesh.shape["fs"], mesh.shape["tp"] // 2, 2),
        ("grp", "fs", "tp_0", "tp_1"),
    )
    return jax.shard_map(
        on_device,
        mesh=split,
        in_specs=(
            P(("grp", "fs"), TP),
            P(TP),
            P(("grp", "fs"), None),
            P(("grp", "fs"), None),
            P(None, "fs", TP),
            P(None, "fs", TP),
            P(None, "fs", TP),
            P("fs", TP),
            P("fs", TP),
            P("fs", TP),
        ),
        out_specs=(
            P(("grp", "fs"), None, TP),
            P(("grp", "fs"), None, TP),
            P(("grp", "fs"), None, TP),
            P("grp", TP),
            P("grp", TP),
            P("grp", TP),
            P(("grp", "fs"), TP),
        ),
        check_vma=False,
    )
```

```python
import jax
import jax.numpy as jnp
from jax import lax
from jax.sharding import Mesh
from jax.sharding import PartitionSpec as P


CAPACITY = 24
TP = ("tp_0", "tp_1")


norm_eps = 1e-05
routed_scale = 2.5


def exchange(array, axis):
    return lax.all_to_all(array, axis, 0, 0, tiled=True)


def rotated(array, axis, by):
    size = lax.axis_size(axis)
    return lax.ppermute(array, axis, [(i, (i + by) % size) for i in range(size)])


def distances(axis):
    size = lax.axis_size(axis)
    return sorted(range(1, size), key=lambda by: -min(by, size - by))


def summed_parts(blocks, axis):
    at = lax.axis_index(axis)
    size = lax.axis_size(axis)
    pick = lambda i: lax.dynamic_index_in_dim(blocks, i % size, 0, keepdims=False)
    parts = [rotated(pick(at + by), axis, by) for by in distances(axis)]
    total = pick(at).astype(jnp.float32)
    for part in parts:
        total = total + part.astype(jnp.float32)
    return total


def swap_cores(array):
    return lax.ppermute(array, "tp_1", [(0, 1), (1, 0)])


def of_core(array, core, dim):
    half = array.shape[dim] // 2
    return lax.dynamic_slice_in_dim(array, core * half, half, axis=dim)


def copy_for_each(array, axis):
    size = lax.axis_size(axis)
    return exchange(jnp.broadcast_to(array[None], (size, *array.shape)), axis)


def tie(array, after):
    return lax.optimization_barrier((array, after))[0]


def with_shared(routed, shared):
    rows = jnp.broadcast_to(shared[None, None], (routed.shape[0], 1, *shared.shape))
    return jnp.concatenate([routed, rows], axis=1)


def layer(
    tokens,
    norm_gain,
    expert_ids,
    route_scores,
    gate_weight,
    up_weight,
    down_weight,
    shared_gate,
    shared_up,
    shared_down,
):
    shards = lax.axis_size("fs")
    chips = lax.axis_size("tp_0")
    core = lax.axis_index("tp_1")
    experts_all, unit_rows, slice_width = gate_weight.shape
    experts_here = experts_all // shards
    experts_core = experts_all // 2
    tok_rows, top_count = expert_ids.shape
    bf16 = jnp.bfloat16
    float32 = jnp.float32

    tok_float = tokens.astype(float32)
    sums = jnp.stack([jnp.sum(tok_float, axis=1), jnp.sum(tok_float * tok_float, axis=1)])
    row_sum, row_squares = jnp.sum(copy_for_each(sums, TP), axis=0)
    full_width = slice_width * lax.axis_size(TP)
    row_mean = row_sum / full_width
    row_var = row_squares / full_width - row_mean * row_mean
    normed = ((tok_float - row_mean[:, None]) * lax.rsqrt(row_var + norm_eps)[:, None]).astype(bf16)

    route_weight = route_scores / jnp.sum(route_scores, axis=1, keepdims=True) * routed_scale
    sent = jnp.concatenate([normed, expert_ids.T.astype(bf16), route_weight.T.astype(bf16)])
    blocks = copy_for_each(sent, "fs")

    gain = norm_gain[None, None, :]
    both_new = jnp.concatenate(
        [(gate_weight * gain).astype(bf16), (up_weight * gain).astype(bf16)], axis=1
    )
    both_shared = jnp.concatenate([shared_gate * gain[0], shared_up * gain[0]]).astype(bf16)
    down_new = down_weight.astype(bf16)
    down_shared = shared_down.astype(bf16)
    three_new = jnp.concatenate([both_new, down_new], axis=1)
    three_sent = three_new.reshape(shards, experts_here, 3 * unit_rows, slice_width)
    three_sent = with_shared(three_sent, jnp.concatenate([both_shared, down_shared]))
    served = exchange(tie(three_sent, blocks), "fs")

    def over_both(local, shared_local):
        rows = local.shape[1]
        mine = of_core(local, core, 0)
        theirs = jnp.concatenate([of_core(local, 1 - core, 0), shared_local[None]])
        theirs = swap_cores(theirs.reshape(-1, slice_width))
        theirs = theirs.reshape(-1, rows, slice_width)
        theirs_routed = theirs[:-1]
        routed = jnp.concatenate([mine, theirs_routed], axis=2)
        return routed, jnp.concatenate([shared_local, theirs[-1]], axis=1)

    both_pair, both_shared_pair = over_both(both_new, both_shared)
    down_pair, down_shared_pair = over_both(down_new, down_shared)

    blocks = tie(blocks, (both_pair, both_shared_pair, down_pair, down_shared_pair))
    own_tokens = blocks[:, :tok_rows]
    partner_tokens = swap_cores(own_tokens)
    all_tokens = jnp.concatenate([own_tokens, partner_tokens], axis=2)
    ids = blocks[:, tok_rows : tok_rows + top_count].astype(jnp.int32)
    weights = blocks[:, tok_rows + top_count :].astype(float32)

    core_experts = core * experts_core + jnp.arange(experts_core, dtype=jnp.int32)
    named = ids[:, :, None, :] == core_experts[None, None, :, None]
    chosen = jnp.any(named, axis=1)
    weight_of = jnp.sum(jnp.where(named, weights[:, :, None, :], 0.0), axis=1)
    places = jnp.arange(tok_rows, dtype=jnp.int32)
    before = places[:, None] < places[None, :]
    rank = jnp.einsum(
        "bet,tu->beu", chosen.astype(bf16), before.astype(bf16), preferred_element_type=float32
    )
    slot = jnp.where(chosen, rank.astype(jnp.int32), -1)
    in_slot = slot[:, :, None, :] == jnp.arange(CAPACITY, dtype=jnp.int32)[None, None, :, None]
    slots = experts_core * CAPACITY
    select = in_slot.astype(bf16).reshape(shards, slots, tok_rows)
    combine = jnp.where(in_slot, weight_of[:, :, None, :], 0.0).astype(bf16)
    combine = combine.reshape(shards, slots, tok_rows)

    rows_in = jnp.einsum(
        "brt,btd->brd", select, all_tokens, preferred_element_type=float32
    ).astype(bf16)
    rows_in = rows_in.reshape(shards, experts_core, CAPACITY, 2 * slice_width).transpose(1, 0, 2, 3)
    rows_in = rows_in.reshape(experts_core, shards * CAPACITY, 2 * slice_width)
    lanes = tok_rows
    groups = shards * CAPACITY // lanes

    def for_groups(weight):
        return jnp.broadcast_to(weight[:, None], (experts_core, groups, *weight.shape[1:]))

    terms = jnp.einsum(
        "egfd,egrd->egfr",
        for_groups(both_pair),
        rows_in.reshape(experts_core, groups, lanes, 2 * slice_width),
        preferred_element_type=float32,
    )
    terms = terms.astype(bf16).reshape(chips, -1, lanes)
    shared_terms = jnp.einsum(
        "fd,btd->bft",
        both_shared_pair,
        of_core(all_tokens, core, 0),
        preferred_element_type=float32,
    ).astype(bf16)
    share = summed_parts(jnp.concatenate([terms, shared_terms], axis=1), "tp_0")
    share = share.reshape(-1, 2 * unit_rows, lanes)
    part = (jax.nn.silu(share[:, :unit_rows]) * share[:, unit_rows:]).astype(bf16)
    hidden = lax.all_gather(part.reshape(-1, lanes), "tp_0")
    hidden = hidden.reshape(chips, -1, unit_rows, lanes)

    results = jnp.einsum(
        "egfr,egfd->egrd",
        hidden[:, :-1].reshape(experts_core, groups, unit_rows, lanes),
        for_groups(down_pair),
        preferred_element_type=float32,
    ).astype(bf16)
    results = results.reshape(experts_core, shards, CAPACITY, 2 * slice_width).transpose(1, 0, 2, 3)
    results = results.reshape(shards, slots, 2 * slice_width)
    total = jnp.einsum("brt,brd->btd", combine, results, preferred_element_type=float32)
    shared_out = jnp.einsum(
        "bft,fd->btd", hidden[:, -1], down_shared_pair, preferred_element_type=float32
    )
    halves = jnp.arange(shards, dtype=jnp.int32)[:, None, None] // (shards // 2) == core
    total = total + jnp.where(halves, jnp.concatenate([shared_out, shared_out]), 0.0)
    total = total[:, :, :slice_width] + swap_cores(
        total[:, :, slice_width:].astype(bf16).reshape(-1, slice_width)
    ).reshape(shards, tok_rows, slice_width).astype(float32)
    served = tie(served, hidden)
    partials = exchange(tie(total.astype(bf16), served), "fs")
    layer_out = jnp.sum(partials.astype(float32), axis=0).astype(bf16)

    served = served.reshape(shards, experts_here + 1, 3, unit_rows, slice_width)
    served = served.transpose(2, 1, 0, 3, 4).reshape(
        3, experts_here + 1, shards * unit_rows, slice_width
    )
    gate_here, up_here, down_here = served[0], served[1], served[2]
    return (
        gate_here[:experts_here],
        up_here[:experts_here],
        down_here[:experts_here],
        gate_here[experts_here],
        up_here[experts_here],
        down_here[experts_here],
        layer_out,
    )


def solution(mesh):
    split = Mesh(
        mesh.devices.reshape(mesh.shape["grp"], mesh.shape["fs"], mesh.shape["tp"] // 2, 2),
        ("grp", "fs", "tp_0", "tp_1"),
    )
    return jax.shard_map(
        layer,
        mesh=split,
        in_specs=(
            P(("grp", "fs"), TP),
            P(TP),
            P(("grp", "fs"), None),
            P(("grp", "fs"), None),
            P(None, "fs", TP),
            P(None, "fs", TP),
            P(None, "fs", TP),
            P("fs", TP),
            P("fs", TP),
            P("fs", TP),
        ),
        out_specs=(
            P(("grp", "fs"), None, TP),
            P(("grp", "fs"), None, TP),
            P(("grp", "fs"), None, TP),
            P("grp", TP),
            P("grp", TP),
            P("grp", TP),
            P(("grp", "fs"), TP),
        ),
        check_vma=False,
    )
```

```python
import jax
import jax.numpy as jnp
from jax import lax
from jax.sharding import Mesh
from jax.sharding import PartitionSpec as P


CAPACITY = 24
TP = ("tp_0", "tp_1")


norm_eps = 1e-05
routed_scale = 2.5


def exchange(array, axis):
    return lax.all_to_all(array, axis, 0, 0, tiled=True)


def rotated(array, axis, by):
    size = lax.axis_size(axis)
    return lax.ppermute(array, axis, [(i, (i + by) % size) for i in range(size)])


def summed_parts(blocks, axis):
    at = lax.axis_index(axis)
    size = lax.axis_size(axis)
    half_way = size // 2
    cut = blocks.shape[1] // 2
    pick = lambda i: lax.dynamic_index_in_dim(blocks, i % size, 0, keepdims=False)
    far = pick(at + half_way)
    first = rotated(jnp.concatenate([pick(at - 1), far[cut:]]), axis, size - 1)
    total = pick(at).astype(jnp.float32) + first[: -cut].astype(jnp.float32)
    for by in range(half_way - 1, 1, -1):
        total = total + rotated(pick(at + by), axis, by).astype(jnp.float32)
        if by < half_way - 1:
            total = total + rotated(pick(at - by), axis, size - by).astype(jnp.float32)
    total = total + rotated(pick(at + 1), axis, 1).astype(jnp.float32)
    upper = rotated(far[:cut], axis, half_way)
    last = rotated(
        jnp.concatenate([pick(at - half_way + 1), first[-cut:]]), axis, size - half_way + 1
    )
    total = total + last[: -cut].astype(jnp.float32)
    return total + jnp.concatenate([upper, last[-cut:]]).astype(jnp.float32)


def swap_cores(array):
    return lax.ppermute(array, "tp_1", [(0, 1), (1, 0)])


def of_core(array, core, dim):
    half = array.shape[dim] // 2
    return lax.dynamic_slice_in_dim(array, core * half, half, axis=dim)


def copy_for_each(array, axis):
    size = lax.axis_size(axis)
    return exchange(jnp.broadcast_to(array[None], (size, *array.shape)), axis)


def tie(array, after):
    return lax.optimization_barrier((array, after))[0]


def with_shared(routed, shared):
    rows = jnp.broadcast_to(shared[None, None], (routed.shape[0], 1, *shared.shape))
    return jnp.concatenate([routed, rows], axis=1)


def layer(
    tokens,
    norm_gain,
    expert_ids,
    route_scores,
    gate_weight,
    up_weight,
    down_weight,
    shared_gate,
    shared_up,
    shared_down,
):
    shards = lax.axis_size("fs")
    chips = lax.axis_size("tp_0")
    core = lax.axis_index("tp_1")
    experts_all, unit_rows, slice_width = gate_weight.shape
    experts_here = experts_all // shards
    experts_core = experts_all // 2
    tok_rows, top_count = expert_ids.shape
    bf16 = jnp.bfloat16
    float32 = jnp.float32

    tok_float = tokens.astype(float32)
    sums = jnp.stack([jnp.sum(tok_float, axis=1), jnp.sum(tok_float * tok_float, axis=1)])
    row_sum, row_squares = jnp.sum(copy_for_each(sums, TP), axis=0)
    full_width = slice_width * lax.axis_size(TP)
    row_mean = row_sum / full_width
    row_var = row_squares / full_width - row_mean * row_mean
    normed = ((tok_float - row_mean[:, None]) * lax.rsqrt(row_var + norm_eps)[:, None]).astype(bf16)

    route_weight = route_scores / jnp.sum(route_scores, axis=1, keepdims=True) * routed_scale
    sent = jnp.concatenate([normed, expert_ids.T.astype(bf16), route_weight.T.astype(bf16)])
    blocks = copy_for_each(sent, "fs")

    gain = norm_gain[None, None, :]
    both_new = jnp.concatenate(
        [(gate_weight * gain).astype(bf16), (up_weight * gain).astype(bf16)], axis=1
    )
    both_shared = jnp.concatenate([shared_gate * gain[0], shared_up * gain[0]]).astype(bf16)
    down_new = down_weight.astype(bf16)
    down_shared = shared_down.astype(bf16)
    three_new = jnp.concatenate([both_new, down_new], axis=1)
    three_sent = three_new.reshape(shards, experts_here, 3 * unit_rows, slice_width)
    three_sent = with_shared(three_sent, jnp.concatenate([both_shared, down_shared]))
    served = exchange(tie(three_sent, blocks), "fs")

    def over_both(local, shared_local):
        rows = local.shape[1]
        mine = of_core(local, core, 0)
        theirs = jnp.concatenate([of_core(local, 1 - core, 0), shared_local[None]])
        theirs = swap_cores(theirs.reshape(-1, slice_width))
        theirs = theirs.reshape(-1, rows, slice_width)
        theirs_routed = theirs[:-1]
        routed = jnp.concatenate([mine, theirs_routed], axis=2)
        return routed, jnp.concatenate([shared_local, theirs[-1]], axis=1)

    both_pair, both_shared_pair = over_both(both_new, both_shared)
    down_pair, down_shared_pair = over_both(down_new, down_shared)

    blocks = tie(blocks, (both_pair, both_shared_pair, down_pair, down_shared_pair))
    own_tokens = blocks[:, :tok_rows]
    partner_tokens = swap_cores(own_tokens)
    all_tokens = jnp.concatenate([own_tokens, partner_tokens], axis=2)
    ids = blocks[:, tok_rows : tok_rows + top_count].astype(jnp.int32)
    weights = blocks[:, tok_rows + top_count :].astype(float32)

    core_experts = core * experts_core + jnp.arange(experts_core, dtype=jnp.int32)
    named = ids[:, :, None, :] == core_experts[None, None, :, None]
    chosen = jnp.any(named, axis=1)
    weight_of = jnp.sum(jnp.where(named, weights[:, :, None, :], 0.0), axis=1)
    places = jnp.arange(tok_rows, dtype=jnp.int32)
    before = places[:, None] < places[None, :]
    rank = jnp.einsum(
        "bet,tu->beu", chosen.astype(bf16), before.astype(bf16), preferred_element_type=float32
    )
    slot = jnp.where(chosen, rank.astype(jnp.int32), -1)
    in_slot = slot[:, :, None, :] == jnp.arange(CAPACITY, dtype=jnp.int32)[None, None, :, None]
    slots = experts_core * CAPACITY
    select = in_slot.astype(bf16).reshape(shards, slots, tok_rows)
    combine = jnp.where(in_slot, weight_of[:, :, None, :], 0.0).astype(bf16)
    combine = combine.reshape(shards, slots, tok_rows)

    rows_in = jnp.einsum(
        "brt,btd->brd", select, all_tokens, preferred_element_type=float32
    ).astype(bf16)
    rows_in = rows_in.reshape(shards, experts_core, CAPACITY, 2 * slice_width).transpose(1, 0, 2, 3)
    rows_in = rows_in.reshape(experts_core, shards * CAPACITY, 2 * slice_width)
    lanes = tok_rows
    groups = shards * CAPACITY // lanes

    def for_groups(weight):
        return jnp.broadcast_to(weight[:, None], (experts_core, groups, *weight.shape[1:]))

    terms = jnp.einsum(
        "egfd,egrd->egfr",
        for_groups(both_pair),
        rows_in.reshape(experts_core, groups, lanes, 2 * slice_width),
        preferred_element_type=float32,
    )
    terms = terms.astype(bf16).reshape(chips, -1, lanes)
    shared_terms = jnp.einsum(
        "fd,btd->bft",
        both_shared_pair,
        of_core(all_tokens, core, 0),
        preferred_element_type=float32,
    ).astype(bf16)
    share = summed_parts(jnp.concatenate([terms, shared_terms], axis=1), "tp_0")
    share = share.reshape(-1, 2 * unit_rows, lanes)
    part = (jax.nn.silu(share[:, :unit_rows]) * share[:, unit_rows:]).astype(bf16)
    hidden = lax.all_gather(part.reshape(-1, lanes), "tp_0")
    hidden = hidden.reshape(chips, -1, unit_rows, lanes)

    results = jnp.einsum(
        "egfr,egfd->egrd",
        hidden[:, :-1].reshape(experts_core, groups, unit_rows, lanes),
        for_groups(down_pair),
        preferred_element_type=float32,
    ).astype(bf16)
    results = results.reshape(experts_core, shards, CAPACITY, 2 * slice_width).transpose(1, 0, 2, 3)
    results = results.reshape(shards, slots, 2 * slice_width)
    total = jnp.einsum("brt,brd->btd", combine, results, preferred_element_type=float32)
    shared_out = jnp.einsum(
        "bft,fd->btd", hidden[:, -1], down_shared_pair, preferred_element_type=float32
    )
    halves = jnp.arange(shards, dtype=jnp.int32)[:, None, None] // (shards // 2) == core
    total = total + jnp.where(halves, jnp.concatenate([shared_out, shared_out]), 0.0)
    total = total[:, :, :slice_width] + swap_cores(
        total[:, :, slice_width:].astype(bf16).reshape(-1, slice_width)
    ).reshape(shards, tok_rows, slice_width).astype(float32)
    served = tie(served, hidden)
    partials = exchange(tie(total.astype(bf16), served), "fs")
    layer_out = jnp.sum(partials.astype(float32), axis=0).astype(bf16)

    served = served.reshape(shards, experts_here + 1, 3, unit_rows, slice_width)
    served = served.transpose(2, 1, 0, 3, 4).reshape(
        3, experts_here + 1, shards * unit_rows, slice_width
    )
    gate_here, up_here, down_here = served[0], served[1], served[2]
    return (
        gate_here[:experts_here],
        up_here[:experts_here],
        down_here[:experts_here],
        gate_here[experts_here],
        up_here[experts_here],
        down_here[experts_here],
        layer_out,
    )


def solution(mesh):
    split = Mesh(
        mesh.devices.reshape(mesh.shape["grp"], mesh.shape["fs"], mesh.shape["tp"] // 2, 2),
        ("grp", "fs", "tp_0", "tp_1"),
    )
    return jax.shard_map(
        layer,
        mesh=split,
        in_specs=(
            P(("grp", "fs"), TP),
            P(TP),
            P(("grp", "fs"), None),
            P(("grp", "fs"), None),
            P(None, "fs", TP),
            P(None, "fs", TP),
            P(None, "fs", TP),
            P("fs", TP),
            P("fs", TP),
            P("fs", TP),
        ),
        out_specs=(
            P(("grp", "fs"), None, TP),
            P(("grp", "fs"), None, TP),
            P(("grp", "fs"), None, TP),
            P("grp", TP),
            P("grp", TP),
            P("grp", TP),
            P(("grp", "fs"), TP),
        ),
        check_vma=False,
    )
```

```python
import jax
import jax.numpy as jnp
from jax import lax
from jax.sharding import Mesh
from jax.sharding import PartitionSpec as P


CAPACITY = 24
TP = ("tp_0", "tp_1")
FS = ("fs_0", "fs_1")
NEAR = 4


norm_eps = 1e-05
routed_scale = 2.5


def exchange(array, axis):
    return lax.all_to_all(array, axis, 0, 0, tiled=True)


def rotated(array, axis, by):
    size = lax.axis_size(axis)
    return lax.ppermute(array, axis, [(i, (i + by) % size) for i in range(size)])


def distances(axis):
    size = lax.axis_size(axis)
    return sorted(range(1, size), key=lambda by: -min(by, size - by))


def summed_parts(blocks, axis):
    at = lax.axis_index(axis)
    size = lax.axis_size(axis)
    pick = lambda i: lax.dynamic_index_in_dim(blocks, i % size, 0, keepdims=False)
    parts = [rotated(pick(at + by), axis, by) for by in distances(axis)]
    total = pick(at).astype(jnp.float32)
    for part in parts:
        total = total + part.astype(jnp.float32)
    return total


def swap_cores(array):
    return lax.ppermute(array, "tp_1", [(0, 1), (1, 0)])


def of_core(array, core, dim):
    half = array.shape[dim] // 2
    return lax.dynamic_slice_in_dim(array, core * half, half, axis=dim)


def copy_for_each(array, axis):
    size = lax.axis_size(axis)
    return exchange(jnp.broadcast_to(array[None], (size, *array.shape)), axis)


def tie(array, after):
    return lax.optimization_barrier((array, after))[0]


def with_shared(routed, shared):
    rows = jnp.broadcast_to(shared[None, None], (routed.shape[0], 1, *shared.shape))
    return jnp.concatenate([routed, rows], axis=1)


def layer(
    tokens,
    norm_gain,
    expert_ids,
    route_scores,
    gate_weight,
    up_weight,
    down_weight,
    shared_gate,
    shared_up,
    shared_down,
):
    shards = lax.axis_size(FS)
    far, near = lax.axis_size("fs_0"), lax.axis_size("fs_1")
    chips = lax.axis_size("tp_0")
    core = lax.axis_index("tp_1")
    experts_all, unit_rows, slice_width = gate_weight.shape
    experts_here = experts_all // shards
    experts_core = experts_all // 2
    tok_rows, top_count = expert_ids.shape
    bf16 = jnp.bfloat16
    float32 = jnp.float32

    tok_float = tokens.astype(float32)
    sums = jnp.stack([jnp.sum(tok_float, axis=1), jnp.sum(tok_float * tok_float, axis=1)])
    row_sum, row_squares = jnp.sum(copy_for_each(sums, TP), axis=0)
    full_width = slice_width * lax.axis_size(TP)
    row_mean = row_sum / full_width
    row_var = row_squares / full_width - row_mean * row_mean
    normed = ((tok_float - row_mean[:, None]) * lax.rsqrt(row_var + norm_eps)[:, None]).astype(bf16)

    route_weight = route_scores / jnp.sum(route_scores, axis=1, keepdims=True) * routed_scale
    sent = jnp.concatenate([normed, expert_ids.T.astype(bf16), route_weight.T.astype(bf16)])
    blocks = copy_for_each(sent, "fs_0")
    blocks = copy_for_each(blocks, "fs_1")

    gain = norm_gain[None, None, :]
    both_new = jnp.concatenate(
        [(gate_weight * gain).astype(bf16), (up_weight * gain).astype(bf16)], axis=1
    )
    both_shared = jnp.concatenate([shared_gate * gain[0], shared_up * gain[0]]).astype(bf16)
    down_new = down_weight.astype(bf16)
    down_shared = shared_down.astype(bf16)
    three_new = jnp.concatenate([both_new, down_new], axis=1)
    three_sent = three_new.reshape(shards, experts_here, 3 * unit_rows, slice_width)
    three_sent = with_shared(three_sent, jnp.concatenate([both_shared, down_shared]))
    served = exchange(tie(three_sent, blocks), FS)

    def over_both(local, shared_local):
        rows = local.shape[1]
        mine = of_core(local, core, 0)
        theirs = jnp.concatenate([of_core(local, 1 - core, 0), shared_local[None]])
        theirs = swap_cores(theirs.reshape(-1, slice_width))
        theirs = theirs.reshape(-1, rows, slice_width)
        theirs_routed = theirs[:-1]
        routed = jnp.concatenate([mine, theirs_routed], axis=2)
        return routed, jnp.concatenate([shared_local, theirs[-1]], axis=1)

    both_pair, both_shared_pair = over_both(both_new, both_shared)
    down_pair, down_shared_pair = over_both(down_new, down_shared)

    blocks = tie(blocks, (both_pair, both_shared_pair, down_pair, down_shared_pair))
    blocks = blocks.transpose(1, 0, 2, 3).reshape(shards, *sent.shape)
    own_tokens = blocks[:, :tok_rows]
    partner_tokens = swap_cores(own_tokens)
    all_tokens = jnp.concatenate([own_tokens, partner_tokens], axis=2)
    ids = blocks[:, tok_rows : tok_rows + top_count].astype(jnp.int32)
    weights = blocks[:, tok_rows + top_count :].astype(float32)

    core_experts = core * experts_core + jnp.arange(experts_core, dtype=jnp.int32)
    named = ids[:, :, None, :] == core_experts[None, None, :, None]
    chosen = jnp.any(named, axis=1)
    weight_of = jnp.sum(jnp.where(named, weights[:, :, None, :], 0.0), axis=1)
    places = jnp.arange(tok_rows, dtype=jnp.int32)
    before = places[:, None] < places[None, :]
    rank = jnp.einsum(
        "bet,tu->beu", chosen.astype(bf16), before.astype(bf16), preferred_element_type=float32
    )
    slot = jnp.where(chosen, rank.astype(jnp.int32), -1)
    in_slot = slot[:, :, None, :] == jnp.arange(CAPACITY, dtype=jnp.int32)[None, None, :, None]
    slots = experts_core * CAPACITY
    select = in_slot.astype(bf16).reshape(shards, slots, tok_rows)
    combine = jnp.where(in_slot, weight_of[:, :, None, :], 0.0).astype(bf16)
    combine = combine.reshape(shards, slots, tok_rows)

    rows_in = jnp.einsum(
        "brt,btd->brd", select, all_tokens, preferred_element_type=float32
    ).astype(bf16)
    rows_in = rows_in.reshape(shards, experts_core, CAPACITY, 2 * slice_width).transpose(1, 0, 2, 3)
    rows_in = rows_in.reshape(experts_core, shards * CAPACITY, 2 * slice_width)
    lanes = tok_rows
    groups = shards * CAPACITY // lanes

    def for_groups(weight):
        return jnp.broadcast_to(weight[:, None], (experts_core, groups, *weight.shape[1:]))

    terms = jnp.einsum(
        "egfd,egrd->egfr",
        for_groups(both_pair),
        rows_in.reshape(experts_core, groups, lanes, 2 * slice_width),
        preferred_element_type=float32,
    )
    terms = terms.astype(bf16).reshape(chips, -1, lanes)
    shared_terms = jnp.einsum(
        "fd,btd->bft",
        both_shared_pair,
        of_core(all_tokens, core, 0),
        preferred_element_type=float32,
    ).astype(bf16)
    share = summed_parts(jnp.concatenate([terms, shared_terms], axis=1), "tp_0")
    share = share.reshape(-1, 2 * unit_rows, lanes)
    part = (jax.nn.silu(share[:, :unit_rows]) * share[:, unit_rows:]).astype(bf16)
    hidden = lax.all_gather(part.reshape(-1, lanes), "tp_0")
    hidden = hidden.reshape(chips, -1, unit_rows, lanes)

    results = jnp.einsum(
        "egfr,egfd->egrd",
        hidden[:, :-1].reshape(experts_core, groups, unit_rows, lanes),
        for_groups(down_pair),
        preferred_element_type=float32,
    ).astype(bf16)
    results = results.reshape(experts_core, shards, CAPACITY, 2 * slice_width).transpose(1, 0, 2, 3)
    results = results.reshape(shards, slots, 2 * slice_width)
    total = jnp.einsum("brt,brd->btd", combine, results, preferred_element_type=float32)
    shared_out = jnp.einsum(
        "bft,fd->btd", hidden[:, -1], down_shared_pair, preferred_element_type=float32
    )
    halves = jnp.arange(shards, dtype=jnp.int32)[:, None, None] // (shards // 2) == core
    total = total + jnp.where(halves, jnp.concatenate([shared_out, shared_out]), 0.0)
    total = total[:, :, :slice_width] + swap_cores(
        total[:, :, slice_width:].astype(bf16).reshape(-1, slice_width)
    ).reshape(shards, tok_rows, slice_width).astype(float32)
    served = tie(served, hidden)
    total = total.astype(bf16).reshape(far, near, tok_rows, slice_width).transpose(1, 0, 2, 3)
    partials = exchange(tie(total, served), "fs_1")
    partials = exchange(jnp.sum(partials.astype(float32), axis=0).astype(bf16), "fs_0")
    layer_out = jnp.sum(partials.astype(float32), axis=0).astype(bf16)

    served = served.reshape(shards, experts_here + 1, 3, unit_rows, slice_width)
    served = served.transpose(2, 1, 0, 3, 4).reshape(
        3, experts_here + 1, shards * unit_rows, slice_width
    )
    gate_here, up_here, down_here = served[0], served[1], served[2]
    return (
        gate_here[:experts_here],
        up_here[:experts_here],
        down_here[:experts_here],
        gate_here[experts_here],
        up_here[experts_here],
        down_here[experts_here],
        layer_out,
    )


def solution(mesh):
    groups, shards, width = (mesh.shape[name] for name in ("grp", "fs", "tp"))
    split = Mesh(
        mesh.devices.reshape(groups, shards // NEAR, NEAR, width // 2, 2), ("grp", *FS, *TP)
    )
    return jax.shard_map(
        layer,
        mesh=split,
        in_specs=(
            P(("grp", *FS), TP),
            P(TP),
            P(("grp", *FS), None),
            P(("grp", *FS), None),
            P(None, FS, TP),
            P(None, FS, TP),
            P(None, FS, TP),
            P(FS, TP),
            P(FS, TP),
            P(FS, TP),
        ),
        out_specs=(
            P(("grp", *FS), None, TP),
            P(("grp", *FS), None, TP),
            P(("grp", *FS), None, TP),
            P("grp", TP),
            P("grp", TP),
            P("grp", TP),
            P(("grp", *FS), TP),
        ),
        check_vma=False,
    )
```

```python
import jax
import jax.numpy as jnp
from jax import lax
from jax.sharding import Mesh
from jax.sharding import PartitionSpec as P


CAPACITY = 24
TP = ("tp_0", "tp_1")


norm_eps = 1e-05
routed_scale = 2.5


def exchange(array, axis):
    return lax.all_to_all(array, axis, 0, 0, tiled=True)


def rotated(array, axis, by):
    size = lax.axis_size(axis)
    return lax.ppermute(array, axis, [(i, (i + by) % size) for i in range(size)])


def distances(axis):
    size = lax.axis_size(axis)
    return sorted(range(1, size), key=lambda by: -min(by, size - by))


def summed_parts(blocks, axis):
    at = lax.axis_index(axis)
    size = lax.axis_size(axis)
    pick = lambda i: lax.dynamic_index_in_dim(blocks, i % size, 0, keepdims=False)
    parts = [rotated(pick(at + by), axis, by) for by in distances(axis)]
    total = pick(at).astype(jnp.float32)
    for part in parts:
        total = total + part.astype(jnp.float32)
    return total


def swap_cores(array):
    return lax.ppermute(array, "tp_1", [(0, 1), (1, 0)])


def of_core(array, core, dim):
    half = array.shape[dim] // 2
    return lax.dynamic_slice_in_dim(array, core * half, half, axis=dim)


def copy_for_each(array, axis):
    size = lax.axis_size(axis)
    return exchange(jnp.broadcast_to(array[None], (size, *array.shape)), axis)


def tie(array, after):
    return lax.optimization_barrier((array, after))[0]


def with_shared(routed, shared):
    rows = jnp.broadcast_to(shared[None, None], (routed.shape[0], 1, *shared.shape))
    return jnp.concatenate([routed, rows], axis=1)


def layer(
    tokens,
    norm_gain,
    expert_ids,
    route_scores,
    gate_weight,
    up_weight,
    down_weight,
    shared_gate,
    shared_up,
    shared_down,
):
    shards = lax.axis_size("fs")
    chips = lax.axis_size("tp_0")
    core = lax.axis_index("tp_1")
    experts_all, unit_rows, slice_width = gate_weight.shape
    experts_here = experts_all // shards
    experts_core = experts_all // 2
    tok_rows, top_count = expert_ids.shape
    bf16 = jnp.bfloat16
    float32 = jnp.float32

    tok_float = tokens.astype(float32)
    sums = jnp.concatenate([jnp.sum(tok_float, axis=1), jnp.sum(tok_float * tok_float, axis=1)])
    sums = jnp.sum(copy_for_each(sums, TP), axis=0)
    row_sum, row_squares = sums[:tok_rows], sums[tok_rows:]
    full_width = slice_width * lax.axis_size(TP)
    row_mean = row_sum / full_width
    row_var = row_squares / full_width - row_mean * row_mean
    normed = ((tok_float - row_mean[:, None]) * lax.rsqrt(row_var + norm_eps)[:, None]).astype(bf16)

    route_weight = route_scores / jnp.sum(route_scores, axis=1, keepdims=True) * routed_scale
    sent = jnp.concatenate([normed, expert_ids.T.astype(bf16), route_weight.T.astype(bf16)])
    blocks = copy_for_each(sent, "fs")

    gain = norm_gain[None, None, :]
    both_new = jnp.concatenate(
        [(gate_weight * gain).astype(bf16), (up_weight * gain).astype(bf16)], axis=1
    )
    both_shared = jnp.concatenate([shared_gate * gain[0], shared_up * gain[0]]).astype(bf16)
    down_new = down_weight.astype(bf16)
    down_shared = shared_down.astype(bf16)
    three_new = jnp.concatenate([both_new, down_new], axis=1)
    three_sent = three_new.reshape(shards, experts_here, 3 * unit_rows, slice_width)
    three_sent = with_shared(three_sent, jnp.concatenate([both_shared, down_shared]))
    served = exchange(tie(three_sent, blocks), "fs")

    def over_both(local, shared_local):
        rows = local.shape[1]
        mine = of_core(local, core, 0)
        theirs = jnp.concatenate([of_core(local, 1 - core, 0), shared_local[None]])
        theirs = swap_cores(theirs.reshape(-1, slice_width))
        theirs = theirs.reshape(-1, rows, slice_width)
        theirs_routed = theirs[:-1]
        routed = jnp.concatenate([mine, theirs_routed], axis=2)
        return routed, jnp.concatenate([shared_local, theirs[-1]], axis=1)

    both_pair, both_shared_pair = over_both(both_new, both_shared)
    down_pair, down_shared_pair = over_both(down_new, down_shared)

    blocks = tie(blocks, (both_pair, both_shared_pair, down_pair, down_shared_pair))
    own_tokens = blocks[:, :tok_rows]
    partner_tokens = swap_cores(own_tokens)
    all_tokens = jnp.concatenate([own_tokens, partner_tokens], axis=2)
    ids = blocks[:, tok_rows : tok_rows + top_count].astype(jnp.int32)
    weights = blocks[:, tok_rows + top_count :].astype(float32)

    core_experts = core * experts_core + jnp.arange(experts_core, dtype=jnp.int32)
    named = ids[:, :, None, :] == core_experts[None, None, :, None]
    chosen = jnp.any(named, axis=1)
    weight_of = jnp.sum(jnp.where(named, weights[:, :, None, :], 0.0), axis=1)
    places = jnp.arange(tok_rows, dtype=jnp.int32)
    before = places[:, None] < places[None, :]
    rank = jnp.einsum(
        "bet,tu->beu", chosen.astype(bf16), before.astype(bf16), preferred_element_type=float32
    )
    slot = jnp.where(chosen, rank.astype(jnp.int32), -1)
    in_slot = slot[:, :, None, :] == jnp.arange(CAPACITY, dtype=jnp.int32)[None, None, :, None]
    slots = experts_core * CAPACITY
    select = in_slot.astype(bf16).reshape(shards, slots, tok_rows)
    combine = jnp.where(in_slot, weight_of[:, :, None, :], 0.0).astype(bf16)
    combine = combine.reshape(shards, slots, tok_rows)

    rows_in = jnp.einsum(
        "brt,btd->brd", select, all_tokens, preferred_element_type=float32
    ).astype(bf16)
    rows_in = rows_in.reshape(shards, experts_core, CAPACITY, 2 * slice_width).transpose(1, 0, 2, 3)
    rows_in = rows_in.reshape(experts_core, shards * CAPACITY, 2 * slice_width)
    lanes = tok_rows
    groups = shards * CAPACITY // lanes

    def for_groups(weight):
        return jnp.broadcast_to(weight[:, None], (experts_core, groups, *weight.shape[1:]))

    terms = jnp.einsum(
        "egfd,egrd->egfr",
        for_groups(both_pair),
        rows_in.reshape(experts_core, groups, lanes, 2 * slice_width),
        preferred_element_type=float32,
    )
    terms = terms.astype(bf16).reshape(chips, -1, lanes)
    shared_terms = jnp.einsum(
        "fd,btd->bft",
        both_shared_pair,
        of_core(all_tokens, core, 0),
        preferred_element_type=float32,
    ).astype(bf16)
    share = summed_parts(jnp.concatenate([terms, shared_terms], axis=1), "tp_0")
    share = share.reshape(-1, 2 * unit_rows, lanes)
    part = (jax.nn.silu(share[:, :unit_rows]) * share[:, unit_rows:]).astype(bf16)
    hidden = lax.all_gather(part.reshape(-1, lanes), "tp_0")
    hidden = hidden.reshape(chips, -1, unit_rows, lanes)

    results = jnp.einsum(
        "egfr,egfd->egrd",
        hidden[:, :-1].reshape(experts_core, groups, unit_rows, lanes),
        for_groups(down_pair),
        preferred_element_type=float32,
    ).astype(bf16)
    results = results.reshape(experts_core, shards, CAPACITY, 2 * slice_width).transpose(1, 0, 2, 3)
    results = results.reshape(shards, slots, 2 * slice_width)
    total = jnp.einsum("brt,brd->btd", combine, results, preferred_element_type=float32)
    shared_out = jnp.einsum(
        "bft,fd->btd", hidden[:, -1], down_shared_pair, preferred_element_type=float32
    )
    halves = jnp.arange(shards, dtype=jnp.int32)[:, None, None] // (shards // 2) == core
    total = total + jnp.where(halves, jnp.concatenate([shared_out, shared_out]), 0.0)
    total = total[:, :, :slice_width] + swap_cores(
        total[:, :, slice_width:].astype(bf16).reshape(-1, slice_width)
    ).reshape(shards, tok_rows, slice_width).astype(float32)
    served = tie(served, hidden)
    partials = exchange(tie(total.astype(bf16), served), "fs")
    layer_out = jnp.sum(partials.astype(float32), axis=0).astype(bf16)

    served = served.reshape(shards, experts_here + 1, 3, unit_rows, slice_width)
    served = served.transpose(2, 1, 0, 3, 4).reshape(
        3, experts_here + 1, shards * unit_rows, slice_width
    )
    gate_here, up_here, down_here = served[0], served[1], served[2]
    return (
        gate_here[:experts_here],
        up_here[:experts_here],
        down_here[:experts_here],
        gate_here[experts_here],
        up_here[experts_here],
        down_here[experts_here],
        layer_out,
    )


def solution(mesh):
    split = Mesh(
        mesh.devices.reshape(mesh.shape["grp"], mesh.shape["fs"], mesh.shape["tp"] // 2, 2),
        ("grp", "fs", "tp_0", "tp_1"),
    )
    return jax.shard_map(
        layer,
        mesh=split,
        in_specs=(
            P(("grp", "fs"), TP),
            P(TP),
            P(("grp", "fs"), None),
            P(("grp", "fs"), None),
            P(None, "fs", TP),
            P(None, "fs", TP),
            P(None, "fs", TP),
            P("fs", TP),
            P("fs", TP),
            P("fs", TP),
        ),
        out_specs=(
            P(("grp", "fs"), None, TP),
            P(("grp", "fs"), None, TP),
            P(("grp", "fs"), None, TP),
            P("grp", TP),
            P("grp", TP),
            P("grp", TP),
            P(("grp", "fs"), TP),
        ),
        check_vma=False,
    )
```
